32 devices in a mesh: ep: 8 (over z, x), tp: 4 (over y, core).
Axes of the slice: x: 2, y: 2, z: 4, core: 2. Of those that a mesh axis runs over, the one named last changes fastest.
Arguments:
- out_gate: bfloat16 [8192, 1024], P('ep', 'tp'), may hold values from -6 to 6
- in_gate: bfloat16 [8192, 1024], P('ep', 'tp'), may hold values from -6 to 6
- conv_input: bfloat16 [8192, 1024], P('ep', 'tp'), may hold values from -6 to 6
- conv_taps: float32 [3, 1024], P(None, 'tp'), may hold values from -4 to 4
- group_gain: float32 [1024], P('tp'), may hold values from 0.1 to 1.9
- mix_out_w: bfloat16 [1024, 2048], replicated, may hold values from -0.1875 to 0.1875
- moe_in: bfloat16 [8192, 2048], P(('ep', 'tp')), may hold values from -6 to 6
- moe_gain: float32 [2048], replicated, may hold values from 0.1 to 1.9
- route_ids: int32 [8192, 2], P(('ep', 'tp')), may hold values from 0 to 31, as said below
- route_weight: float32 [8192, 2], P(('ep', 'tp')), may hold values from 0.1 to 1
- gate_w: bfloat16 [32, 2048, 1024], P(('ep', 'tp')), may hold values from -0.125 to 0.125
- up_w: bfloat16 [32, 2048, 1024], P(('ep', 'tp')), may hold values from -0.125 to 0.125
- down_w: bfloat16 [32, 1024, 2048], P(('ep', 'tp')), may hold values from -0.1875 to 0.1875
Outputs:
- mixed: bfloat16 [8192, 2048], P(('ep', 'tp'))
- moe_out: bfloat16 [8192, 2048], P(('ep', 'tp'))
The draws below stay inside these ranges and needn't reach their ends.
Inputs may be any that keep to these rules, and one draw needn't show every extreme that they name: `route_ids`: the two numbers of a row are different experts of one group: group g holds experts g * 4 to g * 4 + 3. The rows of one device (aligned blocks of 256 rows) name each group in exactly 32 rows and each expert in exactly 16 rows.
All inputs are finite; a program needn't handle non-finite values.
Results may differ from the reference program's by a relative error of at most 0.0071.
Values may be sent and summed in bfloat16 or wider, within the bound.
A program may use at most 128 MiB of HBM per device.

```python
import jax
import jax.numpy as jnp
from jax import lax

D = 2048
CC = 1024
GROUP_CH = 64
TAPS = 3
FE = 1024
TOK_B = 256
GROUPS = 8
EXP_GROUP = 4
EXPERTS = 32
TOKENS_A = 8192
TOKENS_B = 8192


def draw_route_ids(key, part):
    block_count = TOKENS_B // TOK_B
    per_group = TOK_B // GROUPS
    block_keys = jax.random.split(jax.random.fold_in(key, 11), block_count)

    def one_block(block_key):
        order_key, label_key = jax.random.split(block_key)
        slot_of = jax.random.permutation(order_key, TOK_B).astype(jnp.int32)
        group_of = slot_of // per_group
        inner_slot = slot_of % per_group
        first_pick = inner_slot % EXP_GROUP
        shift_by = 1 + inner_slot // EXP_GROUP % (EXP_GROUP - 1)
        second_pick = (first_pick + shift_by) % EXP_GROUP
        label_keys = jax.random.split(label_key, GROUPS)
        labels = jax.vmap(lambda one_key: jax.random.permutation(one_key, EXP_GROUP))(label_keys).astype(jnp.int32)
        first_id = group_of * EXP_GROUP + labels[group_of, first_pick]
        second_id = group_of * EXP_GROUP + labels[group_of, second_pick]
        return jnp.stack([first_id, second_id], axis=1)
    return jax.vmap(one_block)(block_keys).reshape(TOKENS_B, 2).astype(jnp.int32)


def block_scale(own_key, extent, cuts, low, largest):
    loudness, own = 1.0, jax.random.fold_in(own_key, 6)
    for dim, parts in cuts:
        draws = jnp.exp(jax.random.uniform(jax.random.fold_in(own, dim), (parts,), jnp.float32, low / len(cuts), largest / len(cuts)))
        loudness = loudness * jnp.repeat(draws, extent[dim] // parts).reshape([-1 if axis == dim else 1 for axis in range(len(extent))])
    return loudness


def centred(own_key, shape, deviation, bound, pieces=(), dtype=jnp.bfloat16):
    drawn = deviation * jax.random.normal(own_key, shape, jnp.float32)
    if pieces:
        drawn = drawn * block_scale(own_key, shape, pieces, -0.22, 0.18)
    return jnp.clip(drawn, -bound, bound).astype(dtype)


def setup_inputs(seed: int = 0) -> dict:
    keys = jax.random.split(jax.random.key(seed), 14)
    return {
        "out_gate": centred(keys[0], (TOKENS_A, CC), 1.0, 6.0, ((0, 8), (1, 4))),
        "in_gate": centred(keys[1], (TOKENS_A, CC), 1.0, 6.0, ((0, 8), (1, 4))),
        "conv_input": centred(keys[2], (TOKENS_A, CC), 1.0, 6.0, ((0, 8), (1, 4))),
        "conv_taps": centred(keys[3], (TAPS, CC), 0.577, 4.0, ((1, 4),), jnp.float32),
        "group_gain": jnp.clip(1.0 + 0.18 * jax.random.normal(keys[4], (CC,), jnp.float32), 0.1, 1.9),
        "mix_out_w": centred(keys[5], (CC, D), CC ** -0.5, 0.1875),
        "moe_in": centred(keys[6], (TOKENS_B, D), 1.0, 6.0, ((0, 32),)),
        "moe_gain": jnp.clip(1.0 + 0.18 * jax.random.normal(keys[7], (D,), jnp.float32), 0.1, 1.9),
        "route_ids": draw_route_ids(jax.random.fold_in(keys[13], 71), 0),
        "route_weight": jnp.clip(0.1 + 0.9 * jax.random.uniform(keys[9], (TOKENS_B, 2), jnp.float32) ** block_scale(keys[9], (TOKENS_B, 2), ((0, 32),), -0.2, 0.2), 0.1, 1.0),
        "gate_w": centred(keys[10], (EXPERTS, D, FE), D ** -0.5, 0.125, ((0, 32),)),
        "up_w": centred(keys[11], (EXPERTS, D, FE), D ** -0.5, 0.125, ((0, 32),)),
        "down_w": centred(keys[12], (EXPERTS, FE, D), FE ** -0.5, 0.1875, ((0, 32),)),
    }


def conv_mixer(out_gate, in_gate, conv_input, conv_taps, group_gain, mix_out_w):
    product = in_gate.astype(jnp.float32) * conv_input.astype(jnp.float32)
    length = product.shape[0]
    padded = jnp.pad(product, ((TAPS - 1, 0), (0, 0)))
    convolved = jnp.zeros_like(product)
    for tap in range(TAPS):
        convolved = convolved + conv_taps[tap] * padded[tap:tap + length]
    gated = out_gate.astype(jnp.float32) * convolved
    grouped = gated.reshape(length, CC // GROUP_CH, GROUP_CH)
    inv_rms = lax.rsqrt(lax.optimization_barrier(jnp.mean(grouped * grouped, axis=-1, keepdims=True)) + 1e-06)
    normed = ((grouped * inv_rms).reshape(length, CC) * group_gain).astype(jnp.bfloat16)
    return jnp.dot(normed, mix_out_w, preferred_element_type=jnp.float32).astype(jnp.bfloat16)

def expert_rows(inputs, w_gate, w_up, w_down):
    gate_part = jnp.dot(inputs, w_gate, preferred_element_type=jnp.float32)
    up_part = jnp.dot(inputs, w_up, preferred_element_type=jnp.float32)
    hidden = (jax.nn.silu(gate_part) * up_part).astype(jnp.bfloat16)
    return jnp.dot(hidden, w_down, preferred_element_type=jnp.float32).astype(jnp.bfloat16)

def reference(out_gate, in_gate, conv_input, conv_taps, group_gain, mix_out_w, moe_in, moe_gain, route_ids, route_weight, gate_w, up_w, down_w):
    mixed = conv_mixer(out_gate, in_gate, conv_input, conv_taps, group_gain, mix_out_w)
    wide_in = moe_in.astype(jnp.float32)
    inv_rms = lax.rsqrt(lax.optimization_barrier(jnp.mean(wide_in * wide_in, axis=-1, keepdims=True)) + 1e-06)
    expert_in = (wide_in * inv_rms * moe_gain).astype(jnp.bfloat16)
    flat_ids = route_ids.reshape(-1).astype(jnp.int32)
    sort_order = jnp.argsort(flat_ids).astype(jnp.int32)
    per_expert = flat_ids.shape[0] // EXPERTS
    tokens_of = (sort_order // 2).reshape(EXPERTS, per_expert)

    def one_expert(operands):
        token_rows, w_gate, w_up, w_down = operands
        return expert_rows(expert_in[token_rows], w_gate, w_up, w_down)
    outputs = lax.map(one_expert, (tokens_of, gate_w, up_w, down_w))
    per_assign = jnp.zeros((flat_ids.shape[0], D), jnp.bfloat16).at[sort_order].set(outputs.reshape(-1, D))
    per_assign = per_assign.reshape(-1, 2, D)
    first_out = per_assign[:, 0].astype(jnp.float32)
    second = per_assign[:, 1].astype(jnp.float32)
    moe_out = (first_out * route_weight[:, 0:1] + second * route_weight[:, 1:2]).astype(jnp.bfloat16)
    return (mixed, moe_out)
```

```python
import functools

import jax
import jax.numpy as jnp
from jax import lax
from jax.experimental import pallas as pl
from jax.experimental.pallas import tpu as pltpu
from jax.sharding import PartitionSpec as P

GROUP_CH = 64
MESH = pl.DeviceIdType.MESH
BF16 = jnp.bfloat16
F32 = jnp.float32


def shifted(value, axis, by):
    count = lax.axis_size(axis)
    pairs = [(i, i + by) for i in range(count) if 0 <= i + by < count]
    return lax.ppermute(value, axis, pairs)


def round_up(value, to):
    return (value + to - 1) // to * to


def tdot(a, b):
    return lax.dot_general(a, b, (((0,), (0,)), ((), ())), preferred_element_type=F32)


def experts_kernel(
    n_ep, n_tp, slot, pad_slot, chunks,
    x_ref, gain_ref, ids_ref, rw_ref, wg_hbm, wu_hbm, wd_hbm,
    out_ref,
    wg, wu, wd, norm, place, sorted_rows, landed, picked, xin, hidden, obuf, comb, sums, fin,
    w_sem, d_send, d_recv, p_send, p_recv, r_send, r_recv, f_send, f_recv,
):
    me_e = lax.axis_index("ep")
    me_t = lax.axis_index("tp")
    tok, width = x_ref.shape
    rows = tok // n_ep
    slots = n_tp * pad_slot
    meta = norm.shape[1] - width
    weights = [
        pltpu.make_async_copy(src.at[0], dst, w_sem.at[i])
        for i, (src, dst) in enumerate(((wg_hbm, wg), (wu_hbm, wu), (wd_hbm, wd)))
    ]
    for copy in weights:
        copy.start()

    def ep_peer(k):
        return lax.rem(me_e + k, n_ep)

    def tp_peer(j):
        return lax.rem(me_t + j, n_tp)

    barrier = pltpu.get_barrier_semaphore()
    for k in range(1, n_ep):
        pl.semaphore_signal(
            barrier, inc=1, device_id={"ep": ep_peer(k), "tp": me_t}, device_id_type=MESH
        )
    for j in range(1, n_tp):
        pl.semaphore_signal(
            barrier, inc=1, device_id={"ep": me_e, "tp": tp_peer(j)}, device_id_type=MESH
        )

    experts = n_ep * n_tp
    ids0, ids1 = ids_ref[:, 0:1], ids_ref[:, 1:2]
    lane_e = lax.broadcasted_iota(jnp.int32, (tok, experts), 1)
    hit0 = (ids0 == lane_e).astype(F32)
    hit1 = (ids1 == lane_e).astype(F32)
    both = (hit0 + hit1).astype(BF16)
    lower = (
        lax.broadcasted_iota(jnp.int32, (tok, tok), 1) < lax.broadcasted_iota(jnp.int32, (tok, tok), 0)
    ).astype(BF16)
    before = jnp.dot(lower, both, preferred_element_type=F32)
    rank0 = jnp.sum(before * hit0, axis=1, keepdims=True).astype(jnp.int32)
    rank1 = jnp.sum(before * hit1, axis=1, keepdims=True).astype(jnp.int32)
    group = ids0 // n_tp
    in_group = ((ids0 // n_tp) == (lane_e // n_tp)).astype(F32)
    rank_g = jnp.sum(before * in_group, axis=1, keepdims=True).astype(jnp.int32) // 2
    place[...] = (
        (group * rows + rank_g) == lax.broadcasted_iota(jnp.int32, (tok, tok), 1)
    ).astype(BF16)
    cell0 = (ids0 - group * n_tp) * pad_slot + rank0
    cell1 = (ids1 - group * n_tp) * pad_slot + rank1
    lane_s = lax.broadcasted_iota(jnp.int32, (tok, slots), 1)
    at0 = (cell0 == lane_s).astype(F32)
    at1 = (cell1 == lane_s).astype(F32)
    weight = at0 * rw_ref[:, 0:1] + at1 * rw_ref[:, 1:2]
    high = weight.astype(BF16)
    low = (weight - high.astype(F32)).astype(BF16)
    packed = [high, low, (at0 + at1).astype(BF16)]
    if meta > 3 * slots:
        packed.append(jnp.zeros((tok, meta - 3 * slots), BF16))
    norm[:, width:] = jnp.concatenate(packed, axis=1)

    step = 32

    @pl.loop(0, tok // step)
    def _(i):
        at = pl.ds(pl.multiple_of(i * step, step), step)
        wide = x_ref[at, :].astype(F32)
        scale = lax.rsqrt(jnp.mean(wide * wide, axis=-1, keepdims=True) + 1e-06)
        norm[at, 0:width] = (wide * scale * gain_ref[...]).astype(BF16)

    sorted_rows[...] = tdot(place[...], norm[...]).astype(BF16)

    pl.semaphore_wait(barrier, n_ep - 1 + n_tp - 1)

    dispatch = []
    for k in range(1, n_ep):
        to = ep_peer(k)
        copy = pltpu.make_async_remote_copy(
            src_ref=sorted_rows.at[pl.ds(pl.multiple_of(to * rows, rows), rows)],
            dst_ref=landed.at[k],
            send_sem=d_send.at[k],
            recv_sem=d_recv.at[k],
            device_id={"ep": to, "tp": me_t},
            device_id_type=MESH,
        )
        copy.start()
        dispatch.append(copy)
    landed[0] = sorted_rows[pl.ds(pl.multiple_of(me_e * rows, rows), rows), :]

    spread = {}
    for k in range(n_ep):
        if k:
            dispatch[k - 1].wait_recv()
        chosen = landed[k, :, pl.ds(width + 2 * slots, slots)]
        picked[k] = tdot(chosen, landed[k, :, 0:width]).astype(BF16)
        for j in range(1, n_tp):
            to = tp_peer(j)
            copy = pltpu.make_async_remote_copy(
                src_ref=picked.at[k, pl.ds(pl.multiple_of(to * pad_slot, pad_slot), pad_slot)],
                dst_ref=xin.at[pl.ds((k * n_tp + j) * pad_slot, pad_slot)],
                send_sem=p_send.at[k, j],
                recv_sem=p_recv.at[k, j],
                device_id={"ep": me_e, "tp": to},
                device_id_type=MESH,
            )
            copy.start()
            spread[k, j] = copy
        xin[pl.ds(k * n_tp * pad_slot, pad_slot), :] = picked[
            k, pl.ds(pl.multiple_of(me_t * pad_slot, pad_slot), pad_slot), :
        ]

    for copy in weights:
        copy.wait()
    hid = wg.shape[1]
    per = n_ep // chunks
    many = per * n_tp * pad_slot
    back = {}
    mine = pl.ds(pl.multiple_of(me_t * pad_slot, pad_slot), pad_slot)
    for c in range(chunks):
        for k in range(c * per, (c + 1) * per):
            for j in range(1, n_tp):
                spread[k, j].wait_recv()
        span = pl.ds(c * many, many)

        @pl.loop(0, hid // 256)
        def _(f):
            cols = pl.ds(pl.multiple_of(f * 256, 256), 256)
            gate = jnp.dot(xin[span, :], wg[:, cols], preferred_element_type=F32)
            up = jnp.dot(xin[span, :], wu[:, cols], preferred_element_type=F32)
            hidden[:, cols] = (gate / (1.0 + jnp.exp(-gate)) * up).astype(BF16)

        @pl.loop(0, width // 512)
        def _(f):
            cols = pl.ds(pl.multiple_of(f * 512, 512), 512)
            obuf[span, cols] = jnp.dot(
                hidden[...], wd[:, cols], preferred_element_type=F32
            ).astype(BF16)

        for k in range(c * per, (c + 1) * per):
            for j in range(1, n_tp):
                to = tp_peer(n_tp - j)
                copy = pltpu.make_async_remote_copy(
                    src_ref=obuf.at[pl.ds((k * n_tp + j) * pad_slot, pad_slot)],
                    dst_ref=comb.at[k, mine],
                    send_sem=r_send.at[k, j],
                    recv_sem=r_recv.at[k, j],
                    device_id={"ep": me_e, "tp": to},
                    device_id_type=MESH,
                )
                copy.start()
                back[k, j] = copy
            comb[k, mine, :] = obuf[pl.ds(k * n_tp * pad_slot, pad_slot), :]

    home = []
    here = pl.ds(pl.multiple_of(me_e * rows, rows), rows)
    order = list(range(1, n_ep)) + [0]
    for k in order:
        for j in range(1, n_tp):
            back[k, j].wait_recv()
        total = jnp.dot(
            landed[k, :, pl.ds(width, slots)], comb[k], preferred_element_type=F32
        ) + jnp.dot(
            landed[k, :, pl.ds(width + slots, slots)], comb[k], preferred_element_type=F32
        )
        if k == 0:
            fin[here, :] = total.astype(BF16)
            continue
        sums[k] = total.astype(BF16)
        copy = pltpu.make_async_remote_copy(
            src_ref=sums.at[k],
            dst_ref=fin.at[here],
            send_sem=f_send.at[k],
            recv_sem=f_recv.at[k],
            device_id={"ep": ep_peer(n_ep - k), "tp": me_t},
            device_id_type=MESH,
        )
        copy.start()
        home.append(copy)
    for copy in home:
        copy.wait_recv()

    @pl.loop(0, width // 512)
    def _(f):
        cols = pl.ds(pl.multiple_of(f * 512, 512), 512)
        out_ref[:, cols] = jnp.dot(
            place[...], fin[:, cols], preferred_element_type=F32
        ).astype(BF16)

    for copy in dispatch + list(spread.values()) + list(back.values()) + home:
        copy.wait_send()


def experts(moe_in, moe_gain, route_ids, route_weight, gate_w, up_w, down_w):
    n_ep, n_tp = lax.axis_size("ep"), lax.axis_size("tp")
    tok, width = moe_in.shape
    hid = gate_w.shape[2]
    slot = 2 * tok // (n_ep * n_tp)
    pad_slot = round_up(slot, 16)
    rows = tok // n_ep
    slots = n_tp * pad_slot
    meta = round_up(3 * slots, 128)
    total = n_ep * slots
    chunks = 2
    vm = pl.BlockSpec(memory_space=pltpu.VMEM)
    hbm = pl.BlockSpec(memory_space=pl.ANY)
    dma = pltpu.SemaphoreType.DMA
    return pl.pallas_call(
        functools.partial(experts_kernel, n_ep, n_tp, slot, pad_slot, chunks),
        out_shape=jax.ShapeDtypeStruct((tok, width), BF16),
        in_specs=[vm, vm, vm, vm, hbm, hbm, hbm],
        out_specs=vm,
        scratch_shapes=[
            pltpu.VMEM((width, hid), BF16),
            pltpu.VMEM((width, hid), BF16),
            pltpu.VMEM((hid, width), BF16),
            pltpu.VMEM((tok, width + meta), BF16),
            pltpu.VMEM((tok, tok), BF16),
            pltpu.VMEM((tok, width + meta), BF16),
            pltpu.VMEM((n_ep, rows, width + meta), BF16),
            pltpu.VMEM((n_ep, slots, width), BF16),
            pltpu.VMEM((total, width), BF16),
            pltpu.VMEM((total // chunks, hid), BF16),
            pltpu.VMEM((total, width), BF16),
            pltpu.VMEM((n_ep, slots, width), BF16),
            pltpu.VMEM((n_ep, rows, width), BF16),
            pltpu.VMEM((tok, width), BF16),
            dma((3,)),
            dma((n_ep,)),
            dma((n_ep,)),
            dma((n_ep, n_tp)),
            dma((n_ep, n_tp)),
            dma((n_ep, n_tp)),
            dma((n_ep, n_tp)),
            dma((n_ep,)),
            dma((n_ep,)),
        ],
        compiler_params=pltpu.CompilerParams(
            collective_id=0, has_side_effects=True, vmem_limit_bytes=60 * 1024 * 1024
        ),
        cost_estimate=pl.CostEstimate(
            flops=6 * total * width * hid, bytes_accessed=8 * width * hid, transcendentals=0
        ),
    )(moe_in, moe_gain.reshape(1, width), route_ids, route_weight, gate_w, up_w, down_w)


def shards(
    out_gate,
    in_gate,
    conv_input,
    conv_taps,
    group_gain,
    mix_out_w,
    moe_in,
    moe_gain,
    route_ids,
    route_weight,
    gate_w,
    up_w,
    down_w,
):
    rows_ep, channels = in_gate.shape
    member_count = lax.axis_size("tp")
    group_count = lax.axis_size("ep")
    reach = conv_taps.shape[0] - 1
    edge_rows = jnp.stack([in_gate[rows_ep - reach :], conv_input[rows_ep - reach :]])
    earlier = shifted(edge_rows, "ep", 1)
    product = in_gate.astype(jnp.float32) * conv_input.astype(jnp.float32)
    before_rows = earlier[0].astype(jnp.float32) * earlier[1].astype(jnp.float32)
    padded = jnp.concatenate([before_rows, product], axis=0)
    convolved = jnp.zeros_like(product)
    for tap in range(reach + 1):
        convolved = convolved + conv_taps[tap] * padded[tap : tap + rows_ep]
    gated = out_gate.astype(jnp.float32) * convolved
    grouped = gated.reshape(rows_ep, channels // GROUP_CH, GROUP_CH)
    inv_rms = lax.rsqrt(jnp.mean(grouped * grouped, axis=-1, keepdims=True) + 1e-06)
    normed = ((grouped * inv_rms).reshape(rows_ep, channels) * group_gain).astype(jnp.bfloat16)
    blocks = normed.reshape(member_count, rows_ep // member_count, channels)
    portion = lax.all_to_all(blocks, "tp", split_axis=0, concat_axis=2, tiled=True)
    flat_rows = portion.reshape(-1, portion.shape[2])
    projected = jnp.dot(flat_rows, mix_out_w, preferred_element_type=jnp.float32).astype(
        jnp.bfloat16
    )
    mixed = projected.reshape(portion.shape[0], portion.shape[1], -1)
    mixed = mixed.reshape(-1, mixed.shape[2])
    moe_out = experts(moe_in, moe_gain, route_ids, route_weight, gate_w, up_w, down_w)
    return (mixed, moe_out)


def solution(mesh):
    in_specs = (
        P("ep", "tp"),
        P("ep", "tp"),
        P("ep", "tp"),
        P(None, "tp"),
        P("tp"),
        P(),
        P(("ep", "tp"), None),
        P(),
        P(("ep", "tp"), None),
        P(("ep", "tp"), None),
        P(("ep", "tp"), None, None),
        P(("ep", "tp"), None, None),
        P(("ep", "tp"), None, None),
    )
    out_specs = (P(("ep", "tp"), None), P(("ep", "tp"), None))
    return jax.shard_map(shards, mesh=mesh, in_specs=in_specs, out_specs=out_specs, check_vma=False)
```

```python
import functools

import jax
import jax.numpy as jnp
from jax import lax
from jax.experimental import pallas as pl
from jax.experimental.pallas import tpu as pltpu
from jax.sharding import PartitionSpec as P

GROUP_CH = 64
MESH = pl.DeviceIdType.MESH
BF16 = jnp.bfloat16
F32 = jnp.float32


def shifted(value, axis, by):
    count = lax.axis_size(axis)
    pairs = [(i, i + by) for i in range(count) if 0 <= i + by < count]
    return lax.ppermute(value, axis, pairs)


def round_up(value, to):
    return (value + to - 1) // to * to


def tdot(a, b):
    return lax.dot_general(a, b, (((0,), (0,)), ((), ())), preferred_element_type=F32)


def experts_kernel(
    n_ep, n_tp, slot, pad_slot, chunks,
    x_ref, gain_ref, ids_ref, rw_ref, normed_ref, wg_hbm, wu_hbm, wd_hbm, wm_hbm,
    mixed_ref, out_ref,
    wg, wu, wd, wm, norm, place, sorted_rows, landed, picked, xin, hidden, comb, sums, fin, mixin,
    w_sem, m_send, m_recv, d_send, d_recv, p_send, p_recv, r_send, r_recv, f_send, f_recv,
):
    me_e = lax.axis_index("ep")
    me_t = lax.axis_index("tp")
    tok, width = x_ref.shape
    rows = tok // n_ep
    slots = n_tp * pad_slot
    meta = norm.shape[1] - width
    weights = [
        pltpu.make_async_copy(src.at[0], dst, w_sem.at[i])
        for i, (src, dst) in enumerate(((wg_hbm, wg), (wu_hbm, wu), (wd_hbm, wd)))
    ]
    weights.append(pltpu.make_async_copy(wm_hbm, wm, w_sem.at[3]))
    for copy in weights:
        copy.start()

    def ep_peer(k):
        return lax.rem(me_e + k, n_ep)

    def tp_peer(j):
        return lax.rem(me_t + j, n_tp)

    barrier = pltpu.get_barrier_semaphore()
    for k in range(1, n_ep):
        pl.semaphore_signal(
            barrier, inc=1, device_id={"ep": ep_peer(k), "tp": me_t}, device_id_type=MESH
        )
    for j in range(1, n_tp):
        pl.semaphore_signal(
            barrier, inc=1, device_id={"ep": me_e, "tp": tp_peer(j)}, device_id_type=MESH
        )

    experts = n_ep * n_tp
    ids0, ids1 = ids_ref[:, 0:1], ids_ref[:, 1:2]
    lane_e = lax.broadcasted_iota(jnp.int32, (tok, experts), 1)
    hit0 = (ids0 == lane_e).astype(F32)
    hit1 = (ids1 == lane_e).astype(F32)
    both = (hit0 + hit1).astype(BF16)
    lower = (
        lax.broadcasted_iota(jnp.int32, (tok, tok), 1) < lax.broadcasted_iota(jnp.int32, (tok, tok), 0)
    ).astype(BF16)
    before = jnp.dot(lower, both, preferred_element_type=F32)
    rank0 = jnp.sum(before * hit0, axis=1, keepdims=True).astype(jnp.int32)
    rank1 = jnp.sum(before * hit1, axis=1, keepdims=True).astype(jnp.int32)
    group = ids0 // n_tp
    in_group = ((ids0 // n_tp) == (lane_e // n_tp)).astype(F32)
    rank_g = jnp.sum(before * in_group, axis=1, keepdims=True).astype(jnp.int32) // 2
    place[...] = (
        (group * rows + rank_g) == lax.broadcasted_iota(jnp.int32, (tok, tok), 1)
    ).astype(BF16)
    cell0 = (ids0 - group * n_tp) * pad_slot + rank0
    cell1 = (ids1 - group * n_tp) * pad_slot + rank1
    lane_s = lax.broadcasted_iota(jnp.int32, (tok, slots), 1)
    at0 = (cell0 == lane_s).astype(F32)
    at1 = (cell1 == lane_s).astype(F32)
    weight = at0 * rw_ref[:, 0:1] + at1 * rw_ref[:, 1:2]
    high = weight.astype(BF16)
    low = (weight - high.astype(F32)).astype(BF16)
    packed = [high, low, (at0 + at1).astype(BF16)]
    if meta > 3 * slots:
        packed.append(jnp.zeros((tok, meta - 3 * slots), BF16))
    norm[:, width:] = jnp.concatenate(packed, axis=1)

    step = 32

    @pl.loop(0, tok // step)
    def _(i):
        at = pl.ds(pl.multiple_of(i * step, step), step)
        wide = x_ref[at, :].astype(F32)
        scale = lax.rsqrt(jnp.mean(wide * wide, axis=-1, keepdims=True) + 1e-06)
        norm[at, 0:width] = (wide * scale * gain_ref[...]).astype(BF16)

    sorted_rows[...] = tdot(place[...], norm[...]).astype(BF16)

    pl.semaphore_wait(barrier, n_ep - 1 + n_tp - 1)

    dispatch = []
    for k in range(1, n_ep):
        to = ep_peer(k)
        copy = pltpu.make_async_remote_copy(
            src_ref=sorted_rows.at[pl.ds(pl.multiple_of(to * rows, rows), rows)],
            dst_ref=landed.at[k],
            send_sem=d_send.at[k],
            recv_sem=d_recv.at[k],
            device_id={"ep": to, "tp": me_t},
            device_id_type=MESH,
        )
        copy.start()
        dispatch.append(copy)
    part, lanes = mixin.shape[0], normed_ref.shape[1]
    own_lanes = pl.ds(pl.multiple_of(me_t * lanes, lanes), lanes)
    mixes = []
    for j in range(1, n_tp):
        to = tp_peer(j)
        copy = pltpu.make_async_remote_copy(
            src_ref=normed_ref.at[pl.ds(pl.multiple_of(to * part, part), part)],
            dst_ref=mixin.at[:, own_lanes],
            send_sem=m_send.at[j],
            recv_sem=m_recv.at[j],
            device_id={"ep": me_e, "tp": to},
            device_id_type=MESH,
        )
        copy.start()
        mixes.append(copy)
    mixin[:, own_lanes] = normed_ref[pl.ds(pl.multiple_of(me_t * part, part), part), :]
    landed[0] = sorted_rows[pl.ds(pl.multiple_of(me_e * rows, rows), rows), :]

    spread = {}
    for k in range(n_ep):
        if k:
            dispatch[k - 1].wait_recv()
        chosen = landed[k, :, pl.ds(width + 2 * slots, slots)]
        picked[k] = tdot(chosen, landed[k, :, 0:width]).astype(BF16)
        for j in range(1, n_tp):
            to = tp_peer(j)
            copy = pltpu.make_async_remote_copy(
                src_ref=picked.at[k, pl.ds(pl.multiple_of(to * pad_slot, pad_slot), pad_slot)],
                dst_ref=xin.at[pl.ds((k * n_tp + j) * pad_slot, pad_slot)],
                send_sem=p_send.at[k, j],
                recv_sem=p_recv.at[k, j],
                device_id={"ep": me_e, "tp": to},
                device_id_type=MESH,
            )
            copy.start()
            spread[k, j] = copy
        xin[pl.ds(k * n_tp * pad_slot, pad_slot), :] = picked[
            k, pl.ds(pl.multiple_of(me_t * pad_slot, pad_slot), pad_slot), :
        ]

    for copy in weights:
        copy.wait()
    for copy in mixes:
        copy.wait_recv()

    @pl.loop(0, width // 512)
    def _(f):
        cols = pl.ds(pl.multiple_of(f * 512, 512), 512)
        mixed_ref[:, cols] = jnp.dot(
            mixin[...], wm[:, cols], preferred_element_type=F32
        ).astype(BF16)

    hid = wg.shape[1]
    per = n_ep // chunks
    many = per * n_tp * pad_slot
    back = {}
    mine = pl.ds(pl.multiple_of(me_t * pad_slot, pad_slot), pad_slot)
    for c in range(chunks):
        for k in range(c * per, (c + 1) * per):
            for j in range(1, n_tp):
                spread[k, j].wait_recv()
        span = pl.ds(c * many, many)

        @pl.loop(0, hid // 256)
        def _(f):
            cols = pl.ds(pl.multiple_of(f * 256, 256), 256)
            gate = jnp.dot(xin[span, :], wg[:, cols], preferred_element_type=F32)
            up = jnp.dot(xin[span, :], wu[:, cols], preferred_element_type=F32)
            hidden[:, cols] = (gate / (1.0 + jnp.exp(-gate)) * up).astype(BF16)

        @pl.loop(0, width // 512)
        def _(f):
            cols = pl.ds(pl.multiple_of(f * 512, 512), 512)
            xin[span, cols] = jnp.dot(
                hidden[...], wd[:, cols], preferred_element_type=F32
            ).astype(BF16)

        for k in range(c * per, (c + 1) * per):
            for j in range(1, n_tp):
                to = tp_peer(n_tp - j)
                copy = pltpu.make_async_remote_copy(
                    src_ref=xin.at[pl.ds((k * n_tp + j) * pad_slot, pad_slot)],
                    dst_ref=comb.at[k, mine],
                    send_sem=r_send.at[k, j],
                    recv_sem=r_recv.at[k, j],
                    device_id={"ep": me_e, "tp": to},
                    device_id_type=MESH,
                )
                copy.start()
                back[k, j] = copy
            comb[k, mine, :] = xin[pl.ds(k * n_tp * pad_slot, pad_slot), :]

    home = []
    here = pl.ds(pl.multiple_of(me_e * rows, rows), rows)
    order = list(range(1, n_ep)) + [0]
    for k in order:
        for j in range(1, n_tp):
            back[k, j].wait_recv()
        total = jnp.dot(
            landed[k, :, pl.ds(width, slots)], comb[k], preferred_element_type=F32
        ) + jnp.dot(
            landed[k, :, pl.ds(width + slots, slots)], comb[k], preferred_element_type=F32
        )
        if k == 0:
            fin[here, :] = total.astype(BF16)
            continue
        sums[k] = total.astype(BF16)
        copy = pltpu.make_async_remote_copy(
            src_ref=sums.at[k],
            dst_ref=fin.at[here],
            send_sem=f_send.at[k],
            recv_sem=f_recv.at[k],
            device_id={"ep": ep_peer(n_ep - k), "tp": me_t},
            device_id_type=MESH,
        )
        copy.start()
        home.append(copy)
    for copy in home:
        copy.wait_recv()

    @pl.loop(0, width // 512)
    def _(f):
        cols = pl.ds(pl.multiple_of(f * 512, 512), 512)
        out_ref[:, cols] = jnp.dot(
            place[...], fin[:, cols], preferred_element_type=F32
        ).astype(BF16)

    for copy in dispatch + list(spread.values()) + list(back.values()) + home + mixes:
        copy.wait_send()


def experts(moe_in, moe_gain, route_ids, route_weight, normed, gate_w, up_w, down_w, mix_out_w):
    n_ep, n_tp = lax.axis_size("ep"), lax.axis_size("tp")
    tok, width = moe_in.shape
    hid = gate_w.shape[2]
    slot = 2 * tok // (n_ep * n_tp)
    pad_slot = round_up(slot, 16)
    rows = tok // n_ep
    slots = n_tp * pad_slot
    meta = round_up(3 * slots, 128)
    total = n_ep * slots
    chunks = 2
    part = normed.shape[0] // n_tp
    channels = mix_out_w.shape[0]
    vm = pl.BlockSpec(memory_space=pltpu.VMEM)
    hbm = pl.BlockSpec(memory_space=pl.ANY)
    dma = pltpu.SemaphoreType.DMA
    return pl.pallas_call(
        functools.partial(experts_kernel, n_ep, n_tp, slot, pad_slot, chunks),
        out_shape=[
            jax.ShapeDtypeStruct((part, width), BF16),
            jax.ShapeDtypeStruct((tok, width), BF16),
        ],
        in_specs=[vm, vm, vm, vm, vm, hbm, hbm, hbm, hbm],
        out_specs=[vm, vm],
        scratch_shapes=[
            pltpu.VMEM((width, hid), BF16),
            pltpu.VMEM((width, hid), BF16),
            pltpu.VMEM((hid, width), BF16),
            pltpu.VMEM((channels, width), BF16),
            pltpu.VMEM((tok, width + meta), BF16),
            pltpu.VMEM((tok, tok), BF16),
            pltpu.VMEM((tok, width + meta), BF16),
            pltpu.VMEM((n_ep, rows, width + meta), BF16),
            pltpu.VMEM((n_ep, slots, width), BF16),
            pltpu.VMEM((total, width), BF16),
            pltpu.VMEM((total // chunks, hid), BF16),
            pltpu.VMEM((n_ep, slots, width), BF16),
            pltpu.VMEM((n_ep, rows, width), BF16),
            pltpu.VMEM((tok, width), BF16),
            pltpu.VMEM((part, channels), BF16),
            dma((4,)),
            dma((n_tp,)),
            dma((n_tp,)),
            dma((n_ep,)),
            dma((n_ep,)),
            dma((n_ep, n_tp)),
            dma((n_ep, n_tp)),
            dma((n_ep, n_tp)),
            dma((n_ep, n_tp)),
            dma((n_ep,)),
            dma((n_ep,)),
        ],
        compiler_params=pltpu.CompilerParams(
            collective_id=0, has_side_effects=True, vmem_limit_bytes=60 * 1024 * 1024
        ),
        cost_estimate=pl.CostEstimate(
            flops=6 * total * width * hid, bytes_accessed=8 * width * hid, transcendentals=0
        ),
    )(moe_in, moe_gain.reshape(1, width), route_ids, route_weight, normed, gate_w, up_w, down_w, mix_out_w)


def shards(
    out_gate,
    in_gate,
    conv_input,
    conv_taps,
    group_gain,
    mix_out_w,
    moe_in,
    moe_gain,
    route_ids,
    route_weight,
    gate_w,
    up_w,
    down_w,
):
    rows_ep, channels = in_gate.shape
    member_count = lax.axis_size("tp")
    group_count = lax.axis_size("ep")
    reach = conv_taps.shape[0] - 1
    edge_rows = jnp.stack([in_gate[rows_ep - reach :], conv_input[rows_ep - reach :]])
    earlier = shifted(edge_rows, "ep", 1)
    product = in_gate.astype(jnp.float32) * conv_input.astype(jnp.float32)
    before_rows = earlier[0].astype(jnp.float32) * earlier[1].astype(jnp.float32)
    padded = jnp.concatenate([before_rows, product], axis=0)
    convolved = jnp.zeros_like(product)
    for tap in range(reach + 1):
        convolved = convolved + conv_taps[tap] * padded[tap : tap + rows_ep]
    gated = out_gate.astype(jnp.float32) * convolved
    grouped = gated.reshape(rows_ep, channels // GROUP_CH, GROUP_CH)
    inv_rms = lax.rsqrt(jnp.mean(grouped * grouped, axis=-1, keepdims=True) + 1e-06)
    normed = ((grouped * inv_rms).reshape(rows_ep, channels) * group_gain).astype(jnp.bfloat16)
    mixed, moe_out = experts(
        moe_in, moe_gain, route_ids, route_weight, normed, gate_w, up_w, down_w, mix_out_w
    )
    return (mixed, moe_out)


def solution(mesh):
    in_specs = (
        P("ep", "tp"),
        P("ep", "tp"),
        P("ep", "tp"),
        P(None, "tp"),
        P("tp"),
        P(),
        P(("ep", "tp"), None),
        P(),
        P(("ep", "tp"), None),
        P(("ep", "tp"), None),
        P(("ep", "tp"), None, None),
        P(("ep", "tp"), None, None),
        P(("ep", "tp"), None, None),
    )
    out_specs = (P(("ep", "tp"), None), P(("ep", "tp"), None))
    return jax.shard_map(shards, mesh=mesh, in_specs=in_specs, out_specs=out_specs, check_vma=False)
```

```python
import functools

import jax
import jax.numpy as jnp
from jax import lax
from jax.experimental import pallas as pl
from jax.experimental.pallas import tpu as pltpu
from jax.sharding import PartitionSpec as P

GROUP_CH = 64
MESH = pl.DeviceIdType.MESH
BF16 = jnp.bfloat16
F32 = jnp.float32


def shifted(value, axis, by):
    count = lax.axis_size(axis)
    pairs = [(i, i + by) for i in range(count) if 0 <= i + by < count]
    return lax.ppermute(value, axis, pairs)


def round_up(value, to):
    return (value + to - 1) // to * to


def tdot(a, b):
    return lax.dot_general(a, b, (((0,), (0,)), ((), ())), preferred_element_type=F32)


def experts_kernel(
    n_ep, n_tp, slot, pad_slot, chunks,
    x_ref, gain_ref, ids_ref, rw_ref, normed_ref, wg_hbm, wu_hbm, wd_hbm, wm_hbm,
    mixed_ref, out_ref,
    wg, wu, wd, wm, norm, place, sorted_rows, landed, picked, xin, hidden, comb, sums, fin, mixin,
    w_sem, m_send, m_recv, d_send, d_recv, p_send, p_recv, r_send, r_recv, f_send, f_recv,
):
    me_e = lax.axis_index("ep")
    me_t = lax.axis_index("tp")
    tok, width = x_ref.shape
    rows = tok // n_ep
    slots = n_tp * pad_slot
    meta = norm.shape[1] - width
    weights = [
        pltpu.make_async_copy(src.at[0], dst, w_sem.at[i])
        for i, (src, dst) in enumerate(((wg_hbm, wg), (wu_hbm, wu), (wd_hbm, wd)))
    ]
    weights.append(pltpu.make_async_copy(wm_hbm, wm, w_sem.at[3]))
    for copy in weights:
        copy.start()

    def ep_peer(k):
        return lax.rem(me_e + k, n_ep)

    def tp_peer(j):
        return lax.rem(me_t + j, n_tp)

    barrier = pltpu.get_barrier_semaphore()
    for k in range(1, n_ep):
        pl.semaphore_signal(
            barrier, inc=1, device_id={"ep": ep_peer(k), "tp": me_t}, device_id_type=MESH
        )
    for j in range(1, n_tp):
        pl.semaphore_signal(
            barrier, inc=1, device_id={"ep": me_e, "tp": tp_peer(j)}, device_id_type=MESH
        )

    experts = n_ep * n_tp
    ids0, ids1 = ids_ref[:, 0:1], ids_ref[:, 1:2]
    lane_e = lax.broadcasted_iota(jnp.int32, (tok, experts), 1)
    hit0 = (ids0 == lane_e).astype(F32)
    hit1 = (ids1 == lane_e).astype(F32)
    both = (hit0 + hit1).astype(BF16)
    lower = (
        lax.broadcasted_iota(jnp.int32, (tok, tok), 1) < lax.broadcasted_iota(jnp.int32, (tok, tok), 0)
    ).astype(BF16)
    before = jnp.dot(lower, both, preferred_element_type=F32)
    rank0 = jnp.sum(before * hit0, axis=1, keepdims=True).astype(jnp.int32)
    rank1 = jnp.sum(before * hit1, axis=1, keepdims=True).astype(jnp.int32)
    group = ids0 // n_tp
    in_group = ((ids0 // n_tp) == (lane_e // n_tp)).astype(F32)
    rank_g = jnp.sum(before * in_group, axis=1, keepdims=True).astype(jnp.int32) // 2
    place[...] = (
        (group * rows + rank_g) == lax.broadcasted_iota(jnp.int32, (tok, tok), 1)
    ).astype(BF16)
    cell0 = (ids0 - group * n_tp) * pad_slot + rank0
    cell1 = (ids1 - group * n_tp) * pad_slot + rank1
    lane_s = lax.broadcasted_iota(jnp.int32, (tok, slots), 1)
    at0 = (cell0 == lane_s).astype(F32)
    at1 = (cell1 == lane_s).astype(F32)
    weight = at0 * rw_ref[:, 0:1] + at1 * rw_ref[:, 1:2]
    high = weight.astype(BF16)
    low = (weight - high.astype(F32)).astype(BF16)
    packed = [high, low, (at0 + at1).astype(BF16)]
    if meta > 3 * slots:
        packed.append(jnp.zeros((tok, meta - 3 * slots), BF16))
    norm[:, width:] = jnp.concatenate(packed, axis=1)

    step = 32

    @pl.loop(0, tok // step)
    def _(i):
        at = pl.ds(pl.multiple_of(i * step, step), step)
        wide = x_ref[at, :].astype(F32)
        scale = lax.rsqrt(jnp.mean(wide * wide, axis=-1, keepdims=True) + 1e-06)
        norm[at, 0:width] = (wide * scale * gain_ref[...]).astype(BF16)

    sorted_rows[...] = tdot(place[...], norm[...]).astype(BF16)

    pl.semaphore_wait(barrier, n_ep - 1 + n_tp - 1)

    dispatch = []
    for k in range(1, n_ep):
        to = ep_peer(k)
        copy = pltpu.make_async_remote_copy(
            src_ref=sorted_rows.at[pl.ds(pl.multiple_of(to * rows, rows), rows)],
            dst_ref=landed.at[k],
            send_sem=d_send.at[k],
            recv_sem=d_recv.at[k],
            device_id={"ep": to, "tp": me_t},
            device_id_type=MESH,
        )
        copy.start()
        dispatch.append(copy)
    part, lanes = mixin.shape[0], normed_ref.shape[1]
    own_lanes = pl.ds(pl.multiple_of(me_t * lanes, lanes), lanes)
    mixes = []
    for j in range(1, n_tp):
        to = tp_peer(j)
        copy = pltpu.make_async_remote_copy(
            src_ref=normed_ref.at[pl.ds(pl.multiple_of(to * part, part), part)],
            dst_ref=mixin.at[:, own_lanes],
            send_sem=m_send.at[j],
            recv_sem=m_recv.at[j],
            device_id={"ep": me_e, "tp": to},
            device_id_type=MESH,
        )
        copy.start()
        mixes.append(copy)
    mixin[:, own_lanes] = normed_ref[pl.ds(pl.multiple_of(me_t * part, part), part), :]
    landed[0] = sorted_rows[pl.ds(pl.multiple_of(me_e * rows, rows), rows), :]

    spread = {}
    for k in range(n_ep):
        if k:
            dispatch[k - 1].wait_recv()
        chosen = landed[k, :, pl.ds(width + 2 * slots, slots)]
        picked[k] = tdot(chosen, landed[k, :, 0:width]).astype(BF16)
        for j in range(1, n_tp):
            to = tp_peer(j)
            copy = pltpu.make_async_remote_copy(
                src_ref=picked.at[k, pl.ds(pl.multiple_of(to * pad_slot, pad_slot), pad_slot)],
                dst_ref=xin.at[pl.ds((k * n_tp + j) * pad_slot, pad_slot)],
                send_sem=p_send.at[k, j],
                recv_sem=p_recv.at[k, j],
                device_id={"ep": me_e, "tp": to},
                device_id_type=MESH,
            )
            copy.start()
            spread[k, j] = copy
        xin[pl.ds(k * n_tp * pad_slot, pad_slot), :] = picked[
            k, pl.ds(pl.multiple_of(me_t * pad_slot, pad_slot), pad_slot), :
        ]

    for copy in weights:
        copy.wait()
    for copy in mixes:
        copy.wait_recv()

    @pl.loop(0, width // 512)
    def _(f):
        cols = pl.ds(pl.multiple_of(f * 512, 512), 512)
        mixed_ref[:, cols] = jnp.dot(
            mixin[...], wm[:, cols], preferred_element_type=F32
        ).astype(BF16)

    hid = wg.shape[1]
    per = n_ep // chunks
    many = per * n_tp * pad_slot
    back = {}
    mine = pl.ds(pl.multiple_of(me_t * pad_slot, pad_slot), pad_slot)
    home = []
    here = pl.ds(pl.multiple_of(me_e * rows, rows), rows)

    def combine(steps):
        for k in steps:
            for j in range(1, n_tp):
                back[k, j].wait_recv()
            total = jnp.dot(
                landed[k, :, pl.ds(width, slots)], comb[k], preferred_element_type=F32
            ) + jnp.dot(
                landed[k, :, pl.ds(width + slots, slots)], comb[k], preferred_element_type=F32
            )
            if k == 0:
                fin[here, :] = total.astype(BF16)
                continue
            sums[k] = total.astype(BF16)
            copy = pltpu.make_async_remote_copy(
                src_ref=sums.at[k],
                dst_ref=fin.at[here],
                send_sem=f_send.at[k],
                recv_sem=f_recv.at[k],
                device_id={"ep": ep_peer(n_ep - k), "tp": me_t},
                device_id_type=MESH,
            )
            copy.start()
            home.append(copy)

    for c in range(chunks):
        for k in range(c * per, (c + 1) * per):
            for j in range(1, n_tp):
                spread[k, j].wait_recv()
        span = pl.ds(c * many, many)

        @pl.loop(0, hid // 256)
        def _(f):
            cols = pl.ds(pl.multiple_of(f * 256, 256), 256)
            gate = jnp.dot(xin[span, :], wg[:, cols], preferred_element_type=F32)
            up = jnp.dot(xin[span, :], wu[:, cols], preferred_element_type=F32)
            hidden[:, cols] = (gate / (1.0 + jnp.exp(-gate)) * up).astype(BF16)

        @pl.loop(0, width // 512)
        def _(f):
            cols = pl.ds(pl.multiple_of(f * 512, 512), 512)
            xin[span, cols] = jnp.dot(
                hidden[...], wd[:, cols], preferred_element_type=F32
            ).astype(BF16)

        for k in range(c * per, (c + 1) * per):
            for j in range(1, n_tp):
                to = tp_peer(n_tp - j)
                copy = pltpu.make_async_remote_copy(
                    src_ref=xin.at[pl.ds((k * n_tp + j) * pad_slot, pad_slot)],
                    dst_ref=comb.at[k, mine],
                    send_sem=r_send.at[k, j],
                    recv_sem=r_recv.at[k, j],
                    device_id={"ep": me_e, "tp": to},
                    device_id_type=MESH,
                )
                copy.start()
                back[k, j] = copy
            comb[k, mine, :] = xin[pl.ds(k * n_tp * pad_slot, pad_slot), :]
        if c:
            combine(range((c - 1) * per, c * per))

    combine(range((chunks - 1) * per, n_ep))
    for copy in home:
        copy.wait_recv()

    @pl.loop(0, width // 512)
    def _(f):
        cols = pl.ds(pl.multiple_of(f * 512, 512), 512)
        out_ref[:, cols] = jnp.dot(
            place[...], fin[:, cols], preferred_element_type=F32
        ).astype(BF16)

    for copy in dispatch + list(spread.values()) + list(back.values()) + home + mixes:
        copy.wait_send()


def experts(moe_in, moe_gain, route_ids, route_weight, normed, gate_w, up_w, down_w, mix_out_w):
    n_ep, n_tp = lax.axis_size("ep"), lax.axis_size("tp")
    tok, width = moe_in.shape
    hid = gate_w.shape[2]
    slot = 2 * tok // (n_ep * n_tp)
    pad_slot = round_up(slot, 16)
    rows = tok // n_ep
    slots = n_tp * pad_slot
    meta = round_up(3 * slots, 128)
    total = n_ep * slots
    chunks = 4
    part = normed.shape[0] // n_tp
    channels = mix_out_w.shape[0]
    vm = pl.BlockSpec(memory_space=pltpu.VMEM)
    hbm = pl.BlockSpec(memory_space=pl.ANY)
    dma = pltpu.SemaphoreType.DMA
    return pl.pallas_call(
        functools.partial(experts_kernel, n_ep, n_tp, slot, pad_slot, chunks),
        out_shape=[
            jax.ShapeDtypeStruct((part, width), BF16),
            jax.ShapeDtypeStruct((tok, width), BF16),
        ],
        in_specs=[vm, vm, vm, vm, vm, hbm, hbm, hbm, hbm],
        out_specs=[vm, vm],
        scratch_shapes=[
            pltpu.VMEM((width, hid), BF16),
            pltpu.VMEM((width, hid), BF16),
            pltpu.VMEM((hid, width), BF16),
            pltpu.VMEM((channels, width), BF16),
            pltpu.VMEM((tok, width + meta), BF16),
            pltpu.VMEM((tok, tok), BF16),
            pltpu.VMEM((tok, width + meta), BF16),
            pltpu.VMEM((n_ep, rows, width + meta), BF16),
            pltpu.VMEM((n_ep, slots, width), BF16),
            pltpu.VMEM((total, width), BF16),
            pltpu.VMEM((total // chunks, hid), BF16),
            pltpu.VMEM((n_ep, slots, width), BF16),
            pltpu.VMEM((n_ep, rows, width), BF16),
            pltpu.VMEM((tok, width), BF16),
            pltpu.VMEM((part, channels), BF16),
            dma((4,)),
            dma((n_tp,)),
            dma((n_tp,)),
            dma((n_ep,)),
            dma((n_ep,)),
            dma((n_ep, n_tp)),
            dma((n_ep, n_tp)),
            dma((n_ep, n_tp)),
            dma((n_ep, n_tp)),
            dma((n_ep,)),
            dma((n_ep,)),
        ],
        compiler_params=pltpu.CompilerParams(
            collective_id=0, has_side_effects=True, vmem_limit_bytes=60 * 1024 * 1024
        ),
        cost_estimate=pl.CostEstimate(
            flops=6 * total * width * hid, bytes_accessed=8 * width * hid, transcendentals=0
        ),
    )(moe_in, moe_gain.reshape(1, width), route_ids, route_weight, normed, gate_w, up_w, down_w, mix_out_w)


def shards(
    out_gate,
    in_gate,
    conv_input,
    conv_taps,
    group_gain,
    mix_out_w,
    moe_in,
    moe_gain,
    route_ids,
    route_weight,
    gate_w,
    up_w,
    down_w,
):
    rows_ep, channels = in_gate.shape
    member_count = lax.axis_size("tp")
    group_count = lax.axis_size("ep")
    reach = conv_taps.shape[0] - 1
    edge_rows = jnp.stack([in_gate[rows_ep - reach :], conv_input[rows_ep - reach :]])
    earlier = shifted(edge_rows, "ep", 1)
    product = in_gate.astype(jnp.float32) * conv_input.astype(jnp.float32)
    before_rows = earlier[0].astype(jnp.float32) * earlier[1].astype(jnp.float32)
    padded = jnp.concatenate([before_rows, product], axis=0)
    convolved = jnp.zeros_like(product)
    for tap in range(reach + 1):
        convolved = convolved + conv_taps[tap] * padded[tap : tap + rows_ep]
    gated = out_gate.astype(jnp.float32) * convolved
    grouped = gated.reshape(rows_ep, channels // GROUP_CH, GROUP_CH)
    inv_rms = lax.rsqrt(jnp.mean(grouped * grouped, axis=-1, keepdims=True) + 1e-06)
    normed = ((grouped * inv_rms).reshape(rows_ep, channels) * group_gain).astype(jnp.bfloat16)
    mixed, moe_out = experts(
        moe_in, moe_gain, route_ids, route_weight, normed, gate_w, up_w, down_w, mix_out_w
    )
    return (mixed, moe_out)


def solution(mesh):
    in_specs = (
        P("ep", "tp"),
        P("ep", "tp"),
        P("ep", "tp"),
        P(None, "tp"),
        P("tp"),
        P(),
        P(("ep", "tp"), None),
        P(),
        P(("ep", "tp"), None),
        P(("ep", "tp"), None),
        P(("ep", "tp"), None, None),
        P(("ep", "tp"), None, None),
        P(("ep", "tp"), None, None),
    )
    out_specs = (P(("ep", "tp"), None), P(("ep", "tp"), None))
    return jax.shard_map(shards, mesh=mesh, in_specs=in_specs, out_specs=out_specs, check_vma=False)
```
